32 devices in a mesh: sp: 8 (over z, x), tp: 4 (over y, core).
Axes of the slice: x: 2, y: 2, z: 4, core: 2. Of those that a mesh axis runs over, the one named last changes fastest.
Arguments:
- layer_grad: bfloat16 [2048, 2048], P('sp', 'tp'), may hold values from -6 to 6
- routes: int32 [2048, 2], P('sp'), may hold values from 0 to 7, all different within a row; in each aligned block of 256 rows (0 to 255, 256 to 511, ...) at most 96 rows name the same one
- route_weights: float32 [2048, 2], P('sp'), may hold values from 0.1 to 0.9
- expert_in: bfloat16 [8, 768, 2048], P('sp', None, 'tp'), may hold values from -50 to 50
- w_gate: bfloat16 [8, 2048, 2048], P('sp', None, 'tp'), may hold values from -0.125 to 0.125
- w_up: bfloat16 [8, 2048, 2048], P('sp', None, 'tp'), may hold values from -0.125 to 0.125
- w_down: bfloat16 [8, 2048, 2048], P('sp', 'tp'), may hold values from -0.125 to 0.125
- conv_in: bfloat16 [2048, 512], P('sp', 'tp'), may hold values from -6 to 6
- c_gate: bfloat16 [2048, 512], P('sp', 'tp'), may hold values from -6 to 6
- b_gate: bfloat16 [2048, 512], P('sp', 'tp'), may hold values from -1.5 to 1.5
- conv_out: bfloat16 [2048, 512], P('sp', 'tp'), may hold values from -1.5 to 1.5
- taps: bfloat16 [3, 512], P(None, 'tp'), may hold values from -3.5 to 3.5
- w_out: bfloat16 [512, 2048], P('tp'), may hold values from -0.25 to 0.25
Outputs:
- grad_w_gate: bfloat16 [8, 2048, 2048], P('sp', None, 'tp')
- grad_w_up: bfloat16 [8, 2048, 2048], P('sp', None, 'tp')
- grad_w_down: bfloat16 [8, 2048, 2048], P('sp', 'tp')
- grad_routed: bfloat16 [2048, 2048], P('sp', 'tp')
- grad_out_proj: float32 [512, 2048], P('tp', 'sp')
- grad_conv_in: bfloat16 [2048, 512], P('sp', 'tp')
- grad_c_gate: bfloat16 [2048, 512], P('sp', 'tp')
- grad_b_gate: bfloat16 [2048, 512], P('sp', 'tp')
The draws below stay inside these ranges and needn't reach their ends.
Inputs may be any that keep to these rules, and one draw needn't show every extreme that they name: `routes`: each token names 2 different experts. Among the tokens of one block of 256, no expert is named more than 96 times, a bound that some block reaches.
All inputs are finite; a program needn't handle non-finite values.
Results may differ from the reference program's by a relative error of at most 0.019.
Values may be sent and summed in bfloat16 or wider, within the bound.
No kernel may reach another device: no remote copies, remote signals or barrier semaphores. Data moves between devices by JAX's collectives and lax.ppermute only.
A program may use at most 64 MiB of HBM per device.

```python
import math
import jax
import jax.numpy as jnp
import numpy as np
from jax import lax

D = 2048
FF = 2048
CW = 512
TAPS = 3
TOP = 2
TOK_DEV = 256
TOKENS = 2048
EXPERTS = 8
CAP = 96
ROWS = 768
N_SP = 8
N_TP = 4


def draw_expert_in(key, part):
    base_key = jax.random.fold_in(key, 7)
    scale_key, value_key = jax.random.split(base_key)
    row_scale = jnp.exp(jax.random.uniform(scale_key, (EXPERTS, ROWS, 1), jnp.float32, math.log(0.3), math.log(3.0)))
    values = jnp.clip(jax.random.normal(value_key, (EXPERTS, ROWS, D), jnp.float32), -5.0, 5.0)
    return (values * row_scale).astype(jnp.bfloat16)


def strengthened(values, stream_key, source, target, shards_of, factor):
    owner, partner = [(jnp.arange(values.shape[axis_at]) // (values.shape[axis_at] // shards_of)).reshape([-1 if axis == axis_at else 1 for axis in range(values.ndim)]) for axis_at in (source, target)]
    chosen = jax.random.permutation(stream_key, shards_of)[partner]
    strong = (owner == chosen) | (owner == (partner + shards_of // 2) % shards_of)
    return jnp.where(strong, factor * values, values)


def block_levels(rng, shape, pieces, low, top_value):
    factor_of, own = 1.0, jax.random.fold_in(rng, 6)
    for axis_at, shards_of in pieces:
        steps = jnp.exp(jax.random.uniform(jax.random.fold_in(own, axis_at), (shards_of,), jnp.float32, low / len(pieces), top_value / len(pieces)))
        factor_of = factor_of * jnp.repeat(steps, shape[axis_at] // shards_of).reshape([-1 if axis == axis_at else 1 for axis in range(len(shape))])
    return factor_of


def shared_out(key, own, number, rows, count, top, reach, lean):
    sequence = jax.random.permutation(key, count)
    packed, ordinary = shares(count, rows * top, reach, lean, True), shares(count, rows * top, reach, lean, False)
    places = jnp.arange(count)

    def named(lengths, rotation):
        used = int((lengths > 0).sum())
        fixed = max(1, used // 4)
        passed = fixed + (places - fixed + rotation * (used - fixed)) % max(1, count - fixed)
        return jnp.zeros((count,), jnp.int32).at[sequence[jnp.where(places < fixed, places, passed)]].set(jnp.asarray(lengths, jnp.int32))

    lengths = jnp.where(number % 4 == 0, named(packed, number // 4), named(ordinary, number - number // 4 - 1))
    mixed = jax.random.permutation(jax.random.fold_in(own, 3), count)
    giver, sink = mixed[0:count // 2 * 2:2], mixed[1:count // 2 * 2:2]
    margin = jnp.minimum(lengths[giver] - 1, reach - lengths[sink]) // 2
    margin = jnp.where((giver == sequence[0]) | (sink == sequence[0]) | (lengths[sink] == 0), 0, jnp.maximum(margin, 0))
    passed = jax.random.randint(jax.random.fold_in(own, 4), (count // 2,), 0, 1 << 20) % (margin + 1)
    lengths = lengths.at[giver].add(-passed).at[sink].add(passed)
    members = jnp.searchsorted(jnp.cumsum(lengths), jnp.arange(rows * top), side="right").astype(jnp.int32)
    table = members.reshape(top, rows).T
    table = table[jax.random.permutation(jax.random.fold_in(own, 1), rows)]
    rotation = jax.random.randint(jax.random.fold_in(own, 2), (rows, 1), 0, top)
    return jnp.take_along_axis(table, (jnp.arange(top)[None, :] + rotation) % top, axis=1)


def shares(number_of, total, limit, skew, full):
    weights = [(1 << 20) // math.isqrt(grade ** skew) + 1 for grade in range(1, number_of + 1)]
    largest = limit if full else min(limit, max(-(-total // number_of), total * weights[0] // sum(weights)))
    least = 1 if total - largest >= number_of - 1 else 0
    counts, rest = [largest] + [least] * (number_of - 1), total - largest - least * (number_of - 1)
    while rest > 0:
        free = [i for i in range(1, number_of) if counts[i] < largest] or [i for i in range(1, number_of) if counts[i] < limit]
        pool, left = sum([weights[i] for i in free]), rest
        for i in free:
            addition = min(limit - counts[i], max(1, left * weights[i] // pool), rest)
            counts[i] = counts[i] + addition
            rest = rest - addition
    return np.array(counts)


def normal_values(key, extent, deviation, most, shards=(), held_as=jnp.bfloat16):
    loudness = block_levels(key, extent, shards, -0.22, 0.18) if shards else 1.0
    result = jax.random.normal(key, extent, jnp.float32) * deviation * loudness
    return jnp.minimum(jnp.maximum(result, -most), most).astype(held_as)


def noise_with(rng, dims, deviation, reach, shards, heavy, held_as=jnp.bfloat16):
    entries = deviation * jax.random.normal(rng, dims, jnp.float32)
    if shards:
        entries = entries * block_levels(rng, dims, shards, -0.22, 0.18)
    return jnp.clip(strengthened(entries, jax.random.fold_in(rng, 3), *heavy), -reach, reach).astype(held_as)


def setup_inputs(seed: int = 0) -> dict:
    key_of = jax.random.split(jax.random.key(seed), 14)
    layer_grad = noise_with(key_of[0], (TOKENS, D), 1.0, 6.0, ((0, 8), (1, 4)), (0, 1, 8, 2.0))
    routes_keys = jax.random.split(jax.random.fold_in(key_of[1], 1), TOKENS // TOK_DEV)
    routes_turns = jax.random.permutation(jax.random.fold_in(key_of[1], 3), TOKENS // TOK_DEV)
    routes = jax.vmap(lambda own, number: shared_out(jax.random.fold_in(key_of[1], 2), own, number, TOK_DEV, EXPERTS, TOP, CAP, 1))(routes_keys, routes_turns).reshape((TOKENS, TOP))
    route_weights = jnp.clip(0.1 + 0.79999997 * jax.random.uniform(key_of[2], (TOKENS, TOP), jnp.float32) ** block_levels(key_of[2], (TOKENS, TOP), ((0, 8),), -0.2, 0.2), 0.1, 0.9)
    expert_in = draw_expert_in(jax.random.fold_in(key_of[13], 71), 0)
    w_gate = normal_values(key_of[4], (EXPERTS, D, FF), D ** -0.5, 0.125, ((0, 8), (2, 4)))
    w_up = normal_values(key_of[5], (EXPERTS, D, FF), D ** -0.5, 0.125, ((0, 8), (2, 4)))
    w_down = normal_values(key_of[6], (EXPERTS, FF, D), FF ** -0.5, 0.125, ((0, 8), (1, 4)))
    conv_in = normal_values(key_of[7], (TOKENS, CW), 1.0, 6.0, ((0, 8), (1, 4)))
    c_gate = normal_values(key_of[8], (TOKENS, CW), 1.0, 6.0, ((0, 8), (1, 4)))
    b_gate = normal_values(key_of[9], (TOKENS, CW), 0.25, 1.5, ((0, 8), (1, 4)))
    conv_out = normal_values(key_of[10], (TOKENS, CW), 0.25, 1.5, ((0, 8), (1, 4)))
    taps = normal_values(key_of[11], (TAPS, CW), TAPS ** -0.5, 3.5, ((1, 4),))
    w_out = normal_values(key_of[12], (CW, D), CW ** -0.5, 0.25, ((0, 4),))
    return dict(layer_grad=layer_grad, routes=routes, route_weights=route_weights, expert_in=expert_in, w_gate=w_gate, w_up=w_up, w_down=w_down, conv_in=conv_in, c_gate=c_gate, b_gate=b_gate, conv_out=conv_out, taps=taps, w_out=w_out)


clamp_limit = 7.0
swish_alpha = 1.702


def slot_rows(routes):
    blocks = routes.reshape(N_SP, TOK_DEV * TOP)
    onehot = (blocks[:, :, None] == jnp.arange(EXPERTS, dtype=jnp.int32)[None, None, :]).astype(jnp.int32)
    slot_rank = jnp.sum((jnp.cumsum(onehot, axis=1) - 1) * onehot, axis=2).astype(jnp.int32)
    source = jnp.arange(N_SP, dtype=jnp.int32)[:, None]
    return (blocks * ROWS + source * CAP + slot_rank).reshape(-1).astype(jnp.int32)


def expert_grads(operands):
    expert_grad, saved_rows, gate_weight, up_weight, down_weight = operands
    gate_pre = jnp.dot(saved_rows, gate_weight, preferred_element_type=jnp.float32)
    up_pre = jnp.dot(saved_rows, up_weight, preferred_element_type=jnp.float32)
    gate_cut = jnp.minimum(gate_pre, clamp_limit)
    up_cut = jnp.clip(up_pre, -clamp_limit, clamp_limit)
    sigmoid_gate = jax.nn.sigmoid(swish_alpha * gate_cut)
    hidden = ((up_cut + 1.0) * gate_cut * sigmoid_gate).astype(jnp.bfloat16)
    act_grad = jnp.dot(expert_grad, down_weight.T, preferred_element_type=jnp.float32)
    grad_down = jnp.dot(hidden.T, expert_grad, preferred_element_type=jnp.float32).astype(jnp.bfloat16)
    slope = sigmoid_gate + swish_alpha * gate_cut * sigmoid_gate * (1.0 - sigmoid_gate)
    gate_grad = jnp.where(gate_pre < clamp_limit, act_grad * (up_cut + 1.0) * slope, 0.0).astype(jnp.bfloat16)
    up_grad = jnp.where(jnp.abs(up_pre) < clamp_limit, act_grad * gate_cut * sigmoid_gate, 0.0).astype(jnp.bfloat16)
    grad_gate = jnp.dot(saved_rows.T, gate_grad, preferred_element_type=jnp.float32).astype(jnp.bfloat16)
    grad_up = jnp.dot(saved_rows.T, up_grad, preferred_element_type=jnp.float32).astype(jnp.bfloat16)
    blocked_gate = gate_grad.astype(jnp.float32).reshape(ROWS, N_TP, FF // N_TP)
    blocked_up = up_grad.astype(jnp.float32).reshape(ROWS, N_TP, FF // N_TP)
    weight_gate = gate_weight.astype(jnp.float32).reshape(D, N_TP, FF // N_TP)
    weight_up = up_weight.astype(jnp.float32).reshape(D, N_TP, FF // N_TP)
    terms = jnp.einsum('rjf,djf->jrd', blocked_gate, weight_gate) + jnp.einsum('rjf,djf->jrd', blocked_up, weight_up)
    rounded = lax.optimization_barrier(terms.astype(jnp.bfloat16))
    input_grad = jnp.sum(rounded.astype(jnp.float32), axis=0).astype(jnp.bfloat16)
    return grad_gate, grad_up, grad_down, input_grad


def reference(layer_grad, routes, route_weights, expert_in, w_gate, w_up, w_down, conv_in, c_gate, b_gate, conv_out, taps, w_out):
    slot_index = slot_rows(routes)
    scaled = (route_weights[:, :, None] * layer_grad[:, None, :].astype(jnp.float32)).astype(jnp.bfloat16)
    scaled = scaled.reshape(TOKENS * TOP, D)
    expert_grad = jnp.zeros((EXPERTS * ROWS, D), jnp.bfloat16).at[slot_index].set(scaled).reshape(EXPERTS, ROWS, D)
    grad_gate, grad_up, grad_down, input_grad = lax.map(expert_grads, (expert_grad, expert_in, w_gate, w_up, w_down))
    picked = input_grad.reshape(EXPERTS * ROWS, D)[slot_index].reshape(TOKENS, TOP, D)
    grad_routed = jnp.sum(picked.astype(jnp.float32), axis=1).astype(jnp.bfloat16)
    mixer_grad = jnp.dot(layer_grad, w_out.T, preferred_element_type=jnp.float32)
    mixed = (b_gate.astype(jnp.float32) * conv_out.astype(jnp.float32)).astype(jnp.bfloat16)
    grad_out_proj = jnp.dot(mixed.T, layer_grad, preferred_element_type=jnp.float32)
    out_grad = mixer_grad * b_gate.astype(jnp.float32)
    padded = jnp.pad(out_grad, ((0, TAPS - 1), (0, 0)))
    tap_values = taps.astype(jnp.float32)
    conv_grad = jnp.zeros((TOKENS, CW), jnp.float32)
    for tap_index in range(TAPS):
        offset = TAPS - 1 - tap_index
        conv_grad = conv_grad + tap_values[tap_index] * padded[offset:offset + TOKENS]
    grad_conv_in = (conv_grad * c_gate.astype(jnp.float32)).astype(jnp.bfloat16)
    grad_c_gate = (conv_grad * conv_in.astype(jnp.float32)).astype(jnp.bfloat16)
    grad_b_gate = (mixer_grad * conv_out.astype(jnp.float32)).astype(jnp.bfloat16)
    return (grad_gate, grad_up, grad_down, grad_routed, grad_out_proj, grad_conv_in, grad_c_gate, grad_b_gate)
```

```python
import functools

import jax
import jax.numpy as jnp
from jax import lax
from jax.experimental import pallas as pl
from jax.experimental.pallas import tpu as pltpu
from jax.sharding import PartitionSpec as P

clamp_limit = 7.0
swish_alpha = 1.702
F32 = jnp.float32
BF16 = jnp.bfloat16
VMEM = pl.BlockSpec(memory_space=pltpu.VMEM)
SMEM = pl.BlockSpec(memory_space=pltpu.SMEM)
params = functools.partial(pltpu.CompilerParams, vmem_limit_bytes=56 * 1024 * 1024)


def cost(flops, moved):
    return pl.CostEstimate(flops=flops, bytes_accessed=moved, transcendentals=0)


def nn(a, b):
    return lax.dot_general(a, b, (((1,), (0,)), ((), ())), preferred_element_type=F32)


def nt(a, b):
    return lax.dot_general(a, b, (((1,), (1,)), ((), ())), preferred_element_type=F32)


def tn(a, b):
    return lax.dot_general(a, b, (((0,), (0,)), ((), ())), preferred_element_type=F32)


def swapped(value, axis, step):
    count = lax.axis_size(axis)
    return lax.ppermute(value, axis, [(i, i ^ step) for i in range(count)])


def passed_along(value, axis, steps):
    count = lax.axis_size(axis)
    leading, last = (max(0, -steps), min(count, count - steps))
    return lax.ppermute(value, axis, [(source, source + steps) for source in range(leading, last)])


def gathered(shard):
    count = lax.axis_size("tp")
    found = [None] * count
    found[0] = shard
    for j in range(2, count, 2):
        found[j] = swapped(shard, "tp", j)
    for j in range(0, count, 2):
        found[j + 1] = swapped(found[j], "tp", 1)
    return found


def reorder_kernel(ids, source, target):
    target[...] = source[...]


def reordered(ids, rows, blocks):
    capacity = rows.shape[0] // blocks
    out = pl.pallas_call(
        reorder_kernel,
        grid_spec=pltpu.PrefetchScalarGridSpec(
            num_scalar_prefetch=1,
            grid=(blocks,),
            in_specs=[pl.BlockSpec((1, capacity, rows.shape[1]), lambda k, ids: (ids[0] ^ k, 0, 0))],
            out_specs=pl.BlockSpec((1, capacity, rows.shape[1]), lambda k, ids: (k, 0, 0)),
        ),
        out_shape=jax.ShapeDtypeStruct((blocks, capacity, rows.shape[1]), BF16),
        compiler_params=params(),
        cost_estimate=cost(1 << 20, 4 * rows.size),
        name="reorder",
    )(ids, rows.reshape(blocks, capacity, rows.shape[1]))
    return out.reshape(rows.shape)


def dispatch_kernel(blocks, capacity, ids, routes, weights, grads, *outs):
    chosen_out, pieces = outs[0], outs[1:]
    tokens = grads.shape[0]
    expert = ids[0] ^ lax.broadcasted_iota(jnp.int32, (blocks, tokens), 0)
    first = jnp.broadcast_to(routes[0:1, :], (blocks, tokens)) == expert
    second = jnp.broadcast_to(routes[1:2, :], (blocks, tokens)) == expert
    member = jnp.where(first | second, 1.0, 0.0)
    weight = jnp.where(first, weights[0:1, :], 0.0) + jnp.where(second, weights[1:2, :], 0.0)
    earlier = lax.broadcasted_iota(jnp.int32, (tokens, tokens), 0) < lax.broadcasted_iota(
        jnp.int32, (tokens, tokens), 1
    )
    rank = nn(member.astype(BF16), jnp.where(earlier, 1.0, 0.0).astype(BF16))
    slot = jnp.where(member > 0.5, rank, -1.0).astype(jnp.int32)
    places = lax.broadcasted_iota(jnp.int32, (capacity, tokens), 0)
    values = grads[...]
    for k in range(blocks):
        hit = jnp.broadcast_to(slot[k : k + 1, :], (capacity, tokens)) == places
        chosen = jnp.where(hit, 1.0, 0.0).astype(BF16)
        chosen_out[k] = chosen
        scale = jnp.sum(
            jnp.where(hit, jnp.broadcast_to(weight[k : k + 1, :], (capacity, tokens)), 0.0),
            axis=1,
            keepdims=True,
        )
        pieces[k][...] = (nn(chosen, values) * scale).astype(BF16)


def dispatched(ids, routes, weights, grads, blocks, capacity):
    tokens, width = grads.shape
    out = pl.pallas_call(
        functools.partial(dispatch_kernel, blocks, capacity),
        in_specs=[SMEM, VMEM, VMEM, VMEM],
        out_specs=[VMEM] * (blocks + 1),
        out_shape=[jax.ShapeDtypeStruct((blocks, capacity, tokens), BF16)]
        + [jax.ShapeDtypeStruct((capacity, width), BF16)] * blocks,
        compiler_params=params(),
        cost_estimate=cost(2 * blocks * capacity * tokens * width, 4 * blocks * capacity * width),
        name="dispatch",
    )(ids, routes.T, weights.T, grads)
    return out[0], out[1:]


def row_block(rows):
    for size in (384, 256, 192, 128, 96):
        if rows % size == 0:
            return size
    return rows


def gate_kernel(count, ids, *refs):
    saved, (w_gate, w_up, hidden, gate_factor, up_factor) = refs[:count], refs[count:]
    width = saved[0].shape[1]
    gate_pre = up_pre = 0.0
    for j in range(count):
        part = pl.ds(pl.multiple_of((ids[1] ^ j) * width, width), width)
        gate_pre += nn(saved[j][...], w_gate[part, :])
        up_pre += nn(saved[j][...], w_up[part, :])
    gate_cut = jnp.minimum(gate_pre, clamp_limit)
    up_cut = jnp.clip(up_pre, -clamp_limit, clamp_limit)
    sig = jax.nn.sigmoid(swish_alpha * gate_cut)
    swish = gate_cut * sig
    hidden[...] = ((up_cut + 1.0) * swish).astype(BF16)
    slope = sig + swish_alpha * swish * (1.0 - sig)
    gate_factor[...] = jnp.where(gate_pre < clamp_limit, (up_cut + 1.0) * slope, 0.0)
    up_factor[...] = jnp.where(jnp.abs(up_pre) < clamp_limit, swish, 0.0)


def gate_stage(ids, saved, w_gate, w_up):
    count, (rows, width) = len(saved), saved[0].shape
    units = w_gate.shape[1]
    size = row_block(rows)
    spec = pl.BlockSpec((size, width), lambda i, ids: (i, 0))
    whole = pl.BlockSpec(w_gate.shape, lambda i, ids: (0, 0))
    out = pl.BlockSpec((size, units), lambda i, ids: (i, 0))
    return pl.pallas_call(
        functools.partial(gate_kernel, count),
        grid_spec=pltpu.PrefetchScalarGridSpec(
            num_scalar_prefetch=1,
            grid=(rows // size,),
            in_specs=[spec] * count + [whole, whole],
            out_specs=[out] * 3,
        ),
        out_shape=[jax.ShapeDtypeStruct((rows, units), d) for d in (BF16, F32, F32)],
        compiler_params=params(),
        cost_estimate=cost(4 * rows * count * width * units, 8 * w_gate.size),
        name="gate_up",
    )(ids, *saved, w_gate, w_up)


def act_kernel(count, ids, *refs):
    grads = refs[:count]
    gate_factor, up_factor, w_down, w_gate, w_up, gate_grad, up_grad, sent = refs[count:]
    width = grads[0].shape[1]

    def part(j):
        return pl.ds(pl.multiple_of((ids[1] ^ j) * width, width), width)

    act = 0.0
    for j in range(count):
        act += nt(grads[j][...], w_down[:, part(j)])
    gate = (act * gate_factor[...]).astype(BF16)
    up = (act * up_factor[...]).astype(BF16)
    gate_grad[...] = gate
    up_grad[...] = up
    for j in range(1, count, 2):
        sent[j // 2] = (nt(gate, w_gate[part(j), :]) + nt(up, w_up[part(j), :])).astype(BF16)


def act_stage(ids, grads, first_row, gate_factor, up_factor, w_down, w_gate, w_up):
    count, (rows, width) = len(grads), grads[0].shape
    units = w_gate.shape[1]
    size = row_block(rows)
    first = first_row // size
    spec = pl.BlockSpec((size, width), lambda i, ids: (i, 0))
    factor = pl.BlockSpec((size, units), lambda i, ids: (i + first, 0))
    out = pl.BlockSpec((size, units), lambda i, ids: (i, 0))
    whole = pl.BlockSpec(w_gate.shape, lambda i, ids: (0, 0))
    down = pl.BlockSpec(w_down.shape, lambda i, ids: (0, 0))
    return pl.pallas_call(
        functools.partial(act_kernel, count),
        grid_spec=pltpu.PrefetchScalarGridSpec(
            num_scalar_prefetch=1,
            grid=(rows // size,),
            in_specs=[spec] * count + [factor, factor, down, whole, whole],
            out_specs=[out, out, pl.BlockSpec((count // 2, size, width), lambda i, ids: (0, i, 0))],
        ),
        out_shape=[
            jax.ShapeDtypeStruct((rows, units), BF16),
            jax.ShapeDtypeStruct((rows, units), BF16),
            jax.ShapeDtypeStruct((count // 2, rows, width), BF16),
        ],
        compiler_params=params(),
        cost_estimate=cost(4 * rows * count * width * units, 12 * w_gate.size),
        name="act",
    )(ids, *grads, gate_factor, up_factor, w_down, w_gate, w_up)


def term_kernel(pairs, ids, gate_grad, up_grad, w_gate, w_up, received, own, *sent):
    width = own.shape[1]
    for i in range(pairs):
        part = pl.ds(pl.multiple_of((ids[1] ^ (2 * i)) * width, width), width)
        term = nt(gate_grad[...], w_gate[part, :]) + nt(up_grad[...], w_up[part, :])
        total = term + received[i].astype(F32)
        if i:
            sent[i - 1][...] = total.astype(BF16)
        else:
            own[...] = total


def term_stage(ids, gate_grad, up_grad, w_gate, w_up, received):
    pairs, rows, width = received.shape
    units = w_gate.shape[1]
    size = row_block(rows)
    spec = pl.BlockSpec((size, units), lambda i, ids: (i, 0))
    whole = pl.BlockSpec(w_gate.shape, lambda i, ids: (0, 0))
    out = pl.BlockSpec((size, width), lambda i, ids: (i, 0))
    result = pl.pallas_call(
        functools.partial(term_kernel, pairs),
        grid_spec=pltpu.PrefetchScalarGridSpec(
            num_scalar_prefetch=1,
            grid=(rows // size,),
            in_specs=[spec, spec, whole, whole, pl.BlockSpec((pairs, size, width), lambda i, ids: (0, i, 0))],
            out_specs=[out] * pairs,
        ),
        out_shape=[jax.ShapeDtypeStruct((rows, width), F32)]
        + [jax.ShapeDtypeStruct((rows, width), BF16)] * (pairs - 1),
        compiler_params=params(),
        cost_estimate=cost(4 * rows * pairs * width * units, 8 * w_gate.size),
        name="terms",
    )(ids, gate_grad, up_grad, w_gate, w_up, received)
    return result[0], result[1:]


def add_kernel(count, own, *refs):
    received, outs = refs[:count], refs[count:]
    capacity = outs[0].shape[0]
    for k in range(len(outs)):
        part = pl.ds(k * capacity, capacity)
        total = own[part, :]
        for other in received:
            total += other[part, :].astype(F32)
        outs[k][...] = total.astype(BF16)


def add_stage(own, received, pieces):
    rows, width = own.shape
    return pl.pallas_call(
        functools.partial(add_kernel, len(received)),
        in_specs=[VMEM] * (1 + len(received)),
        out_specs=[VMEM] * pieces,
        out_shape=[jax.ShapeDtypeStruct((rows // pieces, width), BF16)] * pieces,
        compiler_params=params(),
        cost_estimate=cost(rows * width, 8 * rows * width),
        name="add",
    )(own, *received)


def combine_kernel(chosen, *refs):
    pieces, out = refs[:-1], refs[-1]
    total = 0.0
    for k, piece in enumerate(pieces):
        total += tn(chosen[k], piece[...])
    out[...] = total.astype(BF16)


def combined(chosen, pieces):
    tokens, width = chosen.shape[2], pieces[0].shape[1]
    return pl.pallas_call(
        combine_kernel,
        in_specs=[VMEM] * (1 + len(pieces)),
        out_specs=VMEM,
        out_shape=jax.ShapeDtypeStruct((tokens, width), BF16),
        compiler_params=params(),
        cost_estimate=cost(2 * chosen.size * width, 4 * chosen.size),
        name="combine",
    )(chosen, *pieces)


def turned_kernel(count, ids, *refs):
    saved, (gate_grad, up_grad, out_gate, out_up) = refs[:count], refs[count:]
    for j in range(count):
        @pl.when(pl.program_id(0) == j)
        def _(j=j):
            turned = saved[j][...].T
            out_gate[...] = nn(turned, gate_grad[...]).astype(BF16)
            out_up[...] = nn(turned, up_grad[...]).astype(BF16)


def in_weight_grads(ids, saved, gate_grad, up_grad):
    count, (rows, width) = len(saved), saved[0].shape
    units = gate_grad.shape[1]
    out = pl.BlockSpec((width, units), lambda j, ids: (ids[1] ^ j, 0))
    whole = pl.BlockSpec((rows, width), lambda j, ids: (0, 0))
    grad = pl.BlockSpec((rows, units), lambda j, ids: (0, 0))
    return pl.pallas_call(
        functools.partial(turned_kernel, count),
        grid_spec=pltpu.PrefetchScalarGridSpec(
            num_scalar_prefetch=1,
            grid=(count,),
            in_specs=[whole] * count + [grad, grad],
            out_specs=[out, out],
        ),
        out_shape=[jax.ShapeDtypeStruct((count * width, units), BF16)] * 2,
        compiler_params=params(),
        cost_estimate=cost(4 * rows * count * width * units, 8 * rows * width * count),
        name="in_grads",
    )(ids, *saved, gate_grad, up_grad)


def down_kernel(count, ids, *refs):
    grads, (hidden, out_down, turned) = refs[:count], refs[count:]

    @pl.when(pl.program_id(0) == 0)
    def _():
        turned[...] = hidden[...].T

    for j in range(count):
        @pl.when(pl.program_id(0) == j)
        def _(j=j):
            out_down[...] = nn(turned[...], grads[j][...]).astype(BF16)


def down_weight_grad(ids, grads, hidden):
    count, (rows, width) = len(grads), grads[0].shape
    units = hidden.shape[1]
    return pl.pallas_call(
        functools.partial(down_kernel, count),
        grid_spec=pltpu.PrefetchScalarGridSpec(
            num_scalar_prefetch=1,
            grid=(count,),
            in_specs=[pl.BlockSpec((rows, width), lambda j, ids: (0, 0))] * count
            + [pl.BlockSpec((rows, units), lambda j, ids: (0, 0))],
            out_specs=pl.BlockSpec((units, width), lambda j, ids: (0, ids[1] ^ j)),
            scratch_shapes=[pltpu.VMEM((units, rows), BF16)],
        ),
        out_shape=jax.ShapeDtypeStruct((units, count * width), BF16),
        compiler_params=params(),
        cost_estimate=cost(2 * rows * count * width * units, 4 * rows * width * count),
        name="down_grad",
    )(ids, *grads, hidden)


def mixer_kernel(count, blocks, ids, *refs):
    grads, (w_out, b_gate, conv_out, out_grad, grad_b, projected, full) = refs[:count], refs[count:]
    width = grads[0].shape[1]
    mixer = 0.0
    for j in range(count):
        part = pl.ds(pl.multiple_of((ids[1] ^ j) * width, width), width)
        mixer += nt(grads[j][...], w_out[:, part])
        full[:, part] = grads[j][...]
    gate, conv = b_gate[...].astype(F32), conv_out[...].astype(F32)
    out_grad[...] = mixer * gate
    grad_b[...] = (mixer * conv).astype(BF16)
    mixed = (gate * conv).astype(BF16).T
    if len(projected.shape) == 3:
        share = projected.shape[2]
        for k in range(blocks):
            part = pl.ds(pl.multiple_of((ids[0] ^ k) * share, share), share)
            projected[k] = nn(mixed, full[:, part]).astype(BF16)
    else:
        projected[...] = nn(mixed, full[...]).astype(BF16)


def mixer_stage(ids, grads, w_out, b_gate, conv_out, blocks):
    count, (tokens, width) = len(grads), grads[0].shape
    channels, model = w_out.shape
    share = model // blocks
    direct = share % 128 == 0
    shape = (blocks, channels, share) if direct else (channels, model)
    out_grad, grad_b, projected = pl.pallas_call(
        functools.partial(mixer_kernel, count, blocks),
        in_specs=[SMEM] + [VMEM] * (count + 3),
        out_specs=[VMEM] * 3,
        out_shape=[
            jax.ShapeDtypeStruct((tokens, channels), F32),
            jax.ShapeDtypeStruct((tokens, channels), BF16),
            jax.ShapeDtypeStruct(shape, BF16),
        ],
        scratch_shapes=[pltpu.VMEM((tokens, model), BF16)],
        compiler_params=params(),
        cost_estimate=cost(4 * tokens * channels * model, 4 * tokens * model),
        name="mixer",
    )(ids, *grads, w_out, b_gate, conv_out)
    if not direct:
        projected = projected.reshape(channels, blocks, share).transpose(1, 0, 2)
        projected = projected[jnp.arange(blocks) ^ ids[0]]
    return out_grad, grad_b, projected


def per_device(
    layer_grad,
    routes,
    route_weights,
    expert_in,
    w_gate,
    w_up,
    w_down,
    conv_in,
    c_gate,
    b_gate,
    conv_out,
    taps,
    w_out,
):
    blocks = lax.axis_size("sp")
    tok_rows = layer_grad.shape[0]
    capacity = expert_in.shape[1] // blocks
    ids = jnp.stack([lax.axis_index("sp"), lax.axis_index("tp")]).astype(jnp.int32)
    gate_weight, up_weight, down_weight = w_gate[0], w_up[0], w_down[0]

    saved = gathered(reordered(ids, expert_in[0], blocks))
    chosen, pieces = dispatched(ids, routes, route_weights, layer_grad, blocks, capacity)
    half = blocks // 2
    order = (range(half, blocks), range(half))
    arrived = [[pieces[k] if k == 0 else swapped(pieces[k], "sp", k) for k in group] for group in order]
    token_grads = gathered(layer_grad)
    expert_grads = [gathered(jnp.concatenate(group, axis=0)) for group in arrived]

    hidden, gate_factor, up_factor = gate_stage(ids, saved, gate_weight, up_weight)
    out_grad, grad_b_gate, projected = mixer_stage(ids, token_grads, w_out, b_gate, conv_out, blocks)

    gate_grads, up_grads, returned = [], [], [None] * blocks
    for group, grads in zip(order, expert_grads):
        gate_grad, up_grad, sent = act_stage(
            ids, grads, group[0] * capacity, gate_factor, up_factor, down_weight, gate_weight, up_weight
        )
        received = swapped(sent, "tp", 1)
        own, others = term_stage(ids, gate_grad, up_grad, gate_weight, up_weight, received)
        others = [swapped(value, "tp", 2 * (i + 1)) for i, value in enumerate(others)]
        for k, piece in zip(group, add_stage(own, others, len(group))):
            returned[k] = piece if k == 0 else swapped(piece, "sp", k)
        gate_grads.append(gate_grad)
        up_grads.append(up_grad)
    grad_routed = combined(chosen, returned)

    def joined(first, second):
        return jnp.concatenate([second, first], axis=0)

    grad_gate, grad_up = in_weight_grads(ids, saved, joined(*gate_grads), joined(*up_grads))
    grad_down = down_weight_grad(ids, [joined(a, b) for a, b in zip(*expert_grads)], hidden)

    while projected.shape[0] > 1:
        step = projected.shape[0] // 2
        other = swapped(projected[step:], "sp", step)
        projected = projected[:step].astype(F32) + other.astype(F32)
        if step > 1:
            projected = projected.astype(BF16)
    grad_out_proj = projected[0]

    tap_reach = taps.shape[0] - 1
    following = passed_along(out_grad[:tap_reach], "sp", -1)
    extended = jnp.concatenate([out_grad, following], axis=0)
    tap_values = taps.astype(F32)
    conv_grad = jnp.zeros_like(out_grad)
    for tap_index in range(tap_reach + 1):
        offset = tap_reach - tap_index
        conv_grad = conv_grad + tap_values[tap_index] * extended[offset : offset + tok_rows]
    grad_conv_in = (conv_grad * c_gate.astype(F32)).astype(BF16)
    grad_c_gate = (conv_grad * conv_in.astype(F32)).astype(BF16)
    return (
        grad_gate[None],
        grad_up[None],
        grad_down[None],
        grad_routed,
        grad_out_proj,
        grad_conv_in,
        grad_c_gate,
        grad_b_gate,
    )


def solution(mesh):
    in_specs = (
        P("sp", "tp"),
        P("sp", None),
        P("sp", None),
        P("sp", None, "tp"),
        P("sp", None, "tp"),
        P("sp", None, "tp"),
        P("sp", "tp", None),
        P("sp", "tp"),
        P("sp", "tp"),
        P("sp", "tp"),
        P("sp", "tp"),
        P(None, "tp"),
        P("tp", None),
    )
    out_specs = (
        P("sp", None, "tp"),
        P("sp", None, "tp"),
        P("sp", "tp", None),
        P("sp", "tp"),
        P("tp", "sp"),
        P("sp", "tp"),
        P("sp", "tp"),
        P("sp", "tp"),
    )
    return jax.shard_map(
        per_device, mesh=mesh, in_specs=in_specs, out_specs=out_specs, check_vma=False
    )
```

```python
import functools

import jax
import jax.numpy as jnp
from jax import lax
from jax.experimental import pallas as pl
from jax.experimental.pallas import tpu as pltpu
from jax.sharding import PartitionSpec as P

clamp_limit = 7.0
swish_alpha = 1.702
F32 = jnp.float32
BF16 = jnp.bfloat16
VMEM = pl.BlockSpec(memory_space=pltpu.VMEM)
SMEM = pl.BlockSpec(memory_space=pltpu.SMEM)


def params(mebibytes):
    return pltpu.CompilerParams(vmem_limit_bytes=mebibytes * 1024 * 1024)


def cost(flops, moved):
    return pl.CostEstimate(flops=flops, bytes_accessed=moved, transcendentals=0)


def nn(a, b):
    return lax.dot_general(a, b, (((1,), (0,)), ((), ())), preferred_element_type=F32)


def nt(a, b):
    return lax.dot_general(a, b, (((1,), (1,)), ((), ())), preferred_element_type=F32)


def tn(a, b):
    return lax.dot_general(a, b, (((0,), (0,)), ((), ())), preferred_element_type=F32)


def swapped(value, axis, step):
    count = lax.axis_size(axis)
    return lax.ppermute(value, axis, [(i, i ^ step) for i in range(count)])


def passed_along(value, axis, steps):
    count = lax.axis_size(axis)
    leading, last = (max(0, -steps), min(count, count - steps))
    return lax.ppermute(value, axis, [(source, source + steps) for source in range(leading, last)])


def gathered(shard):
    count = lax.axis_size("tp")
    found = [None] * count
    found[0] = shard
    for j in range(2, count, 2):
        found[j] = swapped(shard, "tp", j)
    for j in range(0, count, 2):
        found[j + 1] = swapped(found[j], "tp", 1)
    return found


def reorder_kernel(ids, source, target):
    target[...] = source[...]


def reordered(ids, rows, blocks):
    capacity = rows.shape[0] // blocks
    out = pl.pallas_call(
        reorder_kernel,
        grid_spec=pltpu.PrefetchScalarGridSpec(
            num_scalar_prefetch=1,
            grid=(blocks,),
            in_specs=[pl.BlockSpec((1, capacity, rows.shape[1]), lambda k, ids: (ids[0] ^ k, 0, 0))],
            out_specs=pl.BlockSpec((1, capacity, rows.shape[1]), lambda k, ids: (k, 0, 0)),
        ),
        out_shape=jax.ShapeDtypeStruct((blocks, capacity, rows.shape[1]), BF16),
        compiler_params=params(8),
        cost_estimate=cost(1 << 20, 4 * rows.size),
        name="reorder",
    )(ids, rows.reshape(blocks, capacity, rows.shape[1]))
    return out.reshape(rows.shape)


def dispatch_kernel(blocks, capacity, ids, routes, weights, grads, *outs):
    chosen_out, pieces = outs[0], outs[1:]
    tokens = grads.shape[0]
    expert = ids[0] ^ lax.broadcasted_iota(jnp.int32, (blocks, tokens), 0)
    first = jnp.broadcast_to(routes[0:1, :], (blocks, tokens)) == expert
    second = jnp.broadcast_to(routes[1:2, :], (blocks, tokens)) == expert
    member = jnp.where(first | second, 1.0, 0.0)
    weight = jnp.where(first, weights[0:1, :], 0.0) + jnp.where(second, weights[1:2, :], 0.0)
    earlier = lax.broadcasted_iota(jnp.int32, (tokens, tokens), 0) < lax.broadcasted_iota(
        jnp.int32, (tokens, tokens), 1
    )
    rank = nn(member.astype(BF16), jnp.where(earlier, 1.0, 0.0).astype(BF16))
    slot = jnp.where(member > 0.5, rank, -1.0).astype(jnp.int32)
    places = lax.broadcasted_iota(jnp.int32, (capacity, tokens), 0)
    values = grads[...]
    for k in range(blocks):
        hit = jnp.broadcast_to(slot[k : k + 1, :], (capacity, tokens)) == places
        chosen = jnp.where(hit, 1.0, 0.0).astype(BF16)
        chosen_out[k] = chosen
        scale = jnp.sum(
            jnp.where(hit, jnp.broadcast_to(weight[k : k + 1, :], (capacity, tokens)), 0.0),
            axis=1,
            keepdims=True,
        )
        pieces[k][...] = (nn(chosen, values) * scale).astype(BF16)


def dispatched(ids, routes, weights, grads, blocks, capacity):
    tokens, width = grads.shape
    out = pl.pallas_call(
        functools.partial(dispatch_kernel, blocks, capacity),
        in_specs=[SMEM, VMEM, VMEM, VMEM],
        out_specs=[VMEM] * (blocks + 1),
        out_shape=[jax.ShapeDtypeStruct((blocks, capacity, tokens), BF16)]
        + [jax.ShapeDtypeStruct((capacity, width), BF16)] * blocks,
        compiler_params=params(16),
        cost_estimate=cost(2 * blocks * capacity * tokens * width, 4 * blocks * capacity * width),
        name="dispatch",
    )(ids, routes.T, weights.T, grads)
    return out[0], out[1:]


def row_block(rows):
    for size in (384, 256, 192, 128, 96):
        if rows % size == 0:
            return size
    return rows


def part_of(ids, j, width):
    return pl.ds(pl.multiple_of((ids[1] ^ j) * width, width), width)


def block_of(ids, k, capacity):
    return pl.ds(pl.multiple_of((ids[0] ^ k) * capacity, capacity), capacity)


def gate_kernel(count, blocks, ids, *refs):
    saved, (w_gate, w_up, hidden, gate_factor, up_factor) = refs[:count], refs[count:]
    rows, width = saved[0].shape
    capacity = rows // blocks if blocks else rows
    parts = [part_of(ids, j, width) for j in range(count)]
    size = row_block(rows)
    for begin in range(0, rows, size):
        here = pl.ds(begin, size)
        values = jnp.concatenate([ref[here, :] for ref in saved], axis=1)
        gate_pre = nn(values, jnp.concatenate([w_gate[part, :] for part in parts], axis=0))
        up_pre = nn(values, jnp.concatenate([w_up[part, :] for part in parts], axis=0))
        gate_cut = jnp.minimum(gate_pre, clamp_limit)
        up_cut = jnp.clip(up_pre, -clamp_limit, clamp_limit)
        sig = jax.nn.sigmoid(swish_alpha * gate_cut)
        swish = gate_cut * sig
        slope = sig + swish_alpha * swish * (1.0 - sig)
        results = (
            (hidden, ((up_cut + 1.0) * swish).astype(BF16)),
            (gate_factor, jnp.where(gate_pre < clamp_limit, (up_cut + 1.0) * slope, 0.0)),
            (up_factor, jnp.where(jnp.abs(up_pre) < clamp_limit, swish, 0.0)),
        )
        for ref, value in results:
            if not blocks:
                ref[here, :] = value
                continue
            for low in range(0, size, capacity):
                place = block_of(ids, (begin + low) // capacity, capacity)
                ref[place, :] = value[low : low + capacity, :]


def gate_stage(ids, saved, w_gate, w_up, blocks):
    count, (rows, width) = len(saved), saved[0].shape
    units = w_gate.shape[1]
    return pl.pallas_call(
        functools.partial(gate_kernel, count, blocks),
        in_specs=[SMEM] + [VMEM] * (count + 2),
        out_specs=[VMEM] * 3,
        out_shape=[jax.ShapeDtypeStruct((rows, units), d) for d in (BF16, F32, F32)],
        compiler_params=params(16),
        cost_estimate=cost(4 * rows * count * width * units, 8 * w_gate.size),
        name="gate_up",
    )(ids, *saved, w_gate, w_up)


def act_kernel(count, first, ids, *refs):
    grads = refs[:count]
    gate_factor, up_factor, w_down, w_gate, w_up, gate_grad, up_grad, sent = refs[count:]
    rows, width = grads[0].shape
    parts = [part_of(ids, j, width) for j in range(count)]
    here = pl.ds(first, rows)
    act = nt(
        jnp.concatenate([ref[...] for ref in grads], axis=1),
        jnp.concatenate([w_down[:, part] for part in parts], axis=1),
    )
    gate = (act * gate_factor[here, :]).astype(BF16)
    up = (act * up_factor[here, :]).astype(BF16)
    gate_grad[...] = gate
    up_grad[...] = up
    both = jnp.concatenate([gate, up], axis=1)
    for j in range(1, count, 2):
        weights = jnp.concatenate([w_gate[parts[j], :], w_up[parts[j], :]], axis=1)
        sent[j // 2] = nt(both, weights).astype(BF16)


def act_stage(ids, grads, first, gate_factor, up_factor, w_down, w_gate, w_up):
    count, (rows, width) = len(grads), grads[0].shape
    units = w_gate.shape[1]
    return pl.pallas_call(
        functools.partial(act_kernel, count, first),
        in_specs=[SMEM] + [VMEM] * (count + 5),
        out_specs=[VMEM] * 3,
        out_shape=[
            jax.ShapeDtypeStruct((rows, units), BF16),
            jax.ShapeDtypeStruct((rows, units), BF16),
            jax.ShapeDtypeStruct((count // 2, rows, width), BF16),
        ],
        compiler_params=params(12),
        cost_estimate=cost(4 * rows * count * width * units, 12 * w_gate.size),
        name="act",
    )(ids, *grads, gate_factor, up_factor, w_down, w_gate, w_up)


def term_kernel(pairs, ids, gate_grad, up_grad, w_gate, w_up, received, own, *sent):
    width = own.shape[1]
    both = jnp.concatenate([gate_grad[...], up_grad[...]], axis=1)
    for i in reversed(range(pairs)):
        part = part_of(ids, 2 * i, width)
        weights = jnp.concatenate([w_gate[part, :], w_up[part, :]], axis=1)
        total = nt(both, weights) + received[i].astype(F32)
        if i:
            sent[i - 1][...] = total.astype(BF16)
        else:
            own[...] = total


def term_stage(ids, gate_grad, up_grad, w_gate, w_up, received):
    pairs, rows, width = received.shape
    units = w_gate.shape[1]
    result = pl.pallas_call(
        functools.partial(term_kernel, pairs),
        in_specs=[SMEM] + [VMEM] * 5,
        out_specs=[VMEM] * pairs,
        out_shape=[jax.ShapeDtypeStruct((rows, width), F32)]
        + [jax.ShapeDtypeStruct((rows, width), BF16)] * (pairs - 1),
        compiler_params=params(12),
        cost_estimate=cost(4 * rows * pairs * width * units, 8 * w_gate.size),
        name="terms",
    )(ids, gate_grad, up_grad, w_gate, w_up, received)
    return result[0], result[1:]

def add_kernel(count, own, *refs):
    received, outs = refs[:count], refs[count:]
    capacity = outs[0].shape[0]
    for k in range(len(outs)):
        part = pl.ds(k * capacity, capacity)
        total = own[part, :]
        for other in received:
            total += other[part, :].astype(F32)
        outs[k][...] = total.astype(BF16)


def add_stage(own, received, pieces):
    rows, width = own.shape
    return pl.pallas_call(
        functools.partial(add_kernel, len(received)),
        in_specs=[VMEM] * (1 + len(received)),
        out_specs=[VMEM] * pieces,
        out_shape=[jax.ShapeDtypeStruct((rows // pieces, width), BF16)] * pieces,
        compiler_params=params(8),
        cost_estimate=cost(rows * width, 8 * rows * width),
        name="add",
    )(own, *received)


def combine_kernel(chosen, *refs):
    pieces, out = refs[:-1], refs[-1]
    total = 0.0
    for k, piece in enumerate(pieces):
        total += tn(chosen[k], piece[...])
    out[...] = total.astype(BF16)


def combined(chosen, pieces):
    tokens, width = chosen.shape[2], pieces[0].shape[1]
    return pl.pallas_call(
        combine_kernel,
        in_specs=[VMEM] * (1 + len(pieces)),
        out_specs=VMEM,
        out_shape=jax.ShapeDtypeStruct((tokens, width), BF16),
        compiler_params=params(8),
        cost_estimate=cost(2 * chosen.size * width, 4 * chosen.size),
        name="combine",
    )(chosen, *pieces)


def weight_kernel(count, blocks, ids, *refs):
    saved, refs = refs[:count], refs[count:]
    grads, refs = refs[: 2 * count], refs[2 * count :]
    hidden, gates, ups = refs[0], refs[1:3], refs[3:5]
    out_gate, out_up, out_down, both, turned, tiles, downs, sems = refs[5:]
    rows, width = saved[0].shape
    units = hidden.shape[1]
    low = gates[1].shape[0]
    copies = []

    def leave(tile, target):
        copies.append(pltpu.make_async_copy(tile, target, sems.at[len(copies)]))
        copies[-1].start()

    turned[...] = hidden[...].T
    for j in range(count):
        part = part_of(ids, j, width)
        downs[j] = (
            nn(turned[:, low:], grads[j][...]) + nn(turned[:, :low], grads[count + j][...])
        ).astype(BF16)
        leave(downs.at[j], out_down.at[:, part])
    capacity = rows // blocks if blocks else rows
    for side, pair in enumerate((gates, ups)):
        column = slice(side * units, (side + 1) * units)
        for ref, first in zip(pair, (low, 0)):
            if not blocks:
                both[first : first + ref.shape[0], column] = ref[...]
                continue
            for begin in range(0, ref.shape[0], capacity):
                place = block_of(ids, (first + begin) // capacity, capacity)
                both[place, column] = ref[begin : begin + capacity, :]
    for j in range(count):
        part = part_of(ids, j, width)
        result = nn(saved[j][...].T, both[...]).astype(BF16)
        tiles[j, 0] = result[:, :units]
        tiles[j, 1] = result[:, units:]
        leave(tiles.at[j, 0], out_gate.at[part, :])
        leave(tiles.at[j, 1], out_up.at[part, :])
    for copy in copies:
        copy.wait()


def weight_grads(ids, saved, grads, hidden, gate_grads, up_grads, blocks):
    count, (rows, width) = len(saved), saved[0].shape
    units = hidden.shape[1]
    anywhere = pl.BlockSpec(memory_space=pl.ANY)
    model = count * width
    return pl.pallas_call(
        functools.partial(weight_kernel, count, blocks),
        in_specs=[SMEM] + [VMEM] * (3 * count + 5),
        out_specs=[anywhere] * 3,
        out_shape=[jax.ShapeDtypeStruct(s, BF16) for s in ((model, units), (model, units), (units, model))],
        scratch_shapes=[
            pltpu.VMEM((rows, 2 * units), BF16),
            pltpu.VMEM((units, rows), BF16),
            pltpu.VMEM((count, 2, width, units), BF16),
            pltpu.VMEM((count, units, width), BF16),
            pltpu.SemaphoreType.DMA((3 * count,)),
        ],
        compiler_params=params(24),
        cost_estimate=cost(6 * rows * model * units, 12 * rows * model),
        name="weight_grads",
    )(ids, *saved, *grads[0], *grads[1], hidden, *gate_grads, *up_grads)


def mixer_kernel(count, blocks, ids, *refs):
    grads, (w_out, b_gate, conv_out, out_grad, grad_b, projected, full) = refs[:count], refs[count:]
    width = grads[0].shape[1]
    mixer = 0.0
    for j in range(count):
        part = pl.ds(pl.multiple_of((ids[1] ^ j) * width, width), width)
        mixer += nt(grads[j][...], w_out[:, part])
        full[:, part] = grads[j][...]
    gate, conv = b_gate[...].astype(F32), conv_out[...].astype(F32)
    out_grad[...] = mixer * gate
    grad_b[...] = (mixer * conv).astype(BF16)
    mixed = (gate * conv).astype(BF16).T
    if len(projected.shape) == 3:
        share = projected.shape[2]
        for k in range(blocks):
            part = pl.ds(pl.multiple_of((ids[0] ^ k) * share, share), share)
            projected[k] = nn(mixed, full[:, part]).astype(BF16)
    else:
        projected[...] = nn(mixed, full[...]).astype(BF16)


def mixer_stage(ids, grads, w_out, b_gate, conv_out, blocks):
    count, (tokens, width) = len(grads), grads[0].shape
    channels, model = w_out.shape
    share = model // blocks
    direct = share % 128 == 0
    shape = (blocks, channels, share) if direct else (channels, model)
    out_grad, grad_b, projected = pl.pallas_call(
        functools.partial(mixer_kernel, count, blocks),
        in_specs=[SMEM] + [VMEM] * (count + 3),
        out_specs=[VMEM] * 3,
        out_shape=[
            jax.ShapeDtypeStruct((tokens, channels), F32),
            jax.ShapeDtypeStruct((tokens, channels), BF16),
            jax.ShapeDtypeStruct(shape, BF16),
        ],
        scratch_shapes=[pltpu.VMEM((tokens, model), BF16)],
        compiler_params=params(16),
        cost_estimate=cost(4 * tokens * channels * model, 4 * tokens * model),
        name="mixer",
    )(ids, *grads, w_out, b_gate, conv_out)
    if not direct:
        projected = projected.reshape(channels, blocks, share).transpose(1, 0, 2)
        projected = projected[jnp.arange(blocks) ^ ids[0]]
    return out_grad, grad_b, projected


def per_device(
    layer_grad,
    routes,
    route_weights,
    expert_in,
    w_gate,
    w_up,
    w_down,
    conv_in,
    c_gate,
    b_gate,
    conv_out,
    taps,
    w_out,
):
    blocks = lax.axis_size("sp")
    tok_rows = layer_grad.shape[0]
    capacity = expert_in.shape[1] // blocks
    ids = jnp.stack([lax.axis_index("sp"), lax.axis_index("tp")]).astype(jnp.int32)
    gate_weight, up_weight, down_weight = w_gate[0], w_up[0], w_down[0]

    inside = blocks if capacity % 16 == 0 else 0
    rows = expert_in[0] if inside else reordered(ids, expert_in[0], blocks)
    saved = gathered(rows)
    chosen, pieces = dispatched(ids, routes, route_weights, layer_grad, blocks, capacity)
    half = blocks // 2
    order = (range(half, blocks), range(half))
    arrived = [[pieces[k] if k == 0 else swapped(pieces[k], "sp", k) for k in group] for group in order]
    token_grads = gathered(layer_grad)
    expert_grads = [gathered(jnp.concatenate(group, axis=0)) for group in arrived]

    hidden, gate_factor, up_factor = gate_stage(ids, saved, gate_weight, up_weight, inside)
    out_grad, grad_b_gate, projected = mixer_stage(ids, token_grads, w_out, b_gate, conv_out, blocks)

    gate_grads, up_grads, returned = [], [], [None] * blocks
    for group, grads in zip(order, expert_grads):
        gate_grad, up_grad, sent = act_stage(
            ids, grads, group[0] * capacity, gate_factor, up_factor, down_weight, gate_weight, up_weight
        )
        received = swapped(sent, "tp", 1)
        own, others = term_stage(ids, gate_grad, up_grad, gate_weight, up_weight, received)
        others = [swapped(value, "tp", 2 * (i + 1)) for i, value in enumerate(others)]
        for k, piece in zip(group, add_stage(own, others, len(group))):
            returned[k] = piece if k == 0 else swapped(piece, "sp", k)
        gate_grads.append(gate_grad)
        up_grads.append(up_grad)
    grad_routed = combined(chosen, returned)

    grad_gate, grad_up, grad_down = weight_grads(
        ids, saved, expert_grads, hidden, gate_grads, up_grads, inside
    )

    while projected.shape[0] > 1:
        step = projected.shape[0] // 2
        other = swapped(projected[step:], "sp", step)
        projected = projected[:step].astype(F32) + other.astype(F32)
        if step > 1:
            projected = projected.astype(BF16)
    grad_out_proj = projected[0]

    tap_reach = taps.shape[0] - 1
    following = passed_along(out_grad[:tap_reach], "sp", -1)
    extended = jnp.concatenate([out_grad, following], axis=0)
    tap_values = taps.astype(F32)
    conv_grad = jnp.zeros_like(out_grad)
    for tap_index in range(tap_reach + 1):
        offset = tap_reach - tap_index
        conv_grad = conv_grad + tap_values[tap_index] * extended[offset : offset + tok_rows]
    grad_conv_in = (conv_grad * c_gate.astype(F32)).astype(BF16)
    grad_c_gate = (conv_grad * conv_in.astype(F32)).astype(BF16)
    return (
        grad_gate[None],
        grad_up[None],
        grad_down[None],
        grad_routed,
        grad_out_proj,
        grad_conv_in,
        grad_c_gate,
        grad_b_gate,
    )


def solution(mesh):
    in_specs = (
        P("sp", "tp"),
        P("sp", None),
        P("sp", None),
        P("sp", None, "tp"),
        P("sp", None, "tp"),
        P("sp", None, "tp"),
        P("sp", "tp", None),
        P("sp", "tp"),
        P("sp", "tp"),
        P("sp", "tp"),
        P("sp", "tp"),
        P(None, "tp"),
        P("tp", None),
    )
    out_specs = (
        P("sp", None, "tp"),
        P("sp", None, "tp"),
        P("sp", "tp", None),
        P("sp", "tp"),
        P("tp", "sp"),
        P("sp", "tp"),
        P("sp", "tp"),
        P("sp", "tp"),
    )
    return jax.shard_map(
        per_device, mesh=mesh, in_specs=in_specs, out_specs=out_specs, check_vma=False
    )
```
